32 devices in a mesh: fs: 8 (over z, y), tp: 4 (over x, core).
Axes of the slice: x: 2, y: 2, z: 4, core: 2. Of those that a mesh axis runs over, the one named last changes fastest.
Arguments:
- x_late: bfloat16 [6144, 2048], P(('fs', 'tp')), may hold values from -6 to 6
- x_early: bfloat16 [6144, 2048], P(('fs', 'tp')), may hold values from -6 to 6
- w_gate: bfloat16 [2048, 5632], P('fs', 'tp'), may hold values from -0.125 to 0.125
- w_value: bfloat16 [2048, 5632], P('fs', 'tp'), may hold values from -0.125 to 0.125
- conv_taps: float32 [3, 5632], P(None, 'tp'), may hold values from -3 to 3
- grad_hidden: bfloat16 [6144, 5632], P('fs', 'tp'), may hold values from -6 to 6
- sum_gate: float32 [2048, 5632], P('fs', 'tp'), may hold values from -6 to 6
- sum_value: float32 [2048, 5632], P('fs', 'tp'), may hold values from -6 to 6
- sum_taps: float32 [3, 5632], P(None, 'tp'), may hold values from -6 to 6
Outputs:
- hidden_late: bfloat16 [6144, 5632], P('fs', 'tp')
- grad_early: bfloat16 [6144, 2048], P(('fs', 'tp'))
- new_sum_gate: float32 [2048, 5632], P('fs', 'tp')
- new_sum_value: float32 [2048, 5632], P('fs', 'tp')
- new_sum_taps: float32 [3, 5632], P(None, 'tp')
The draws below stay inside these ranges and needn't reach their ends.
All inputs are finite; a program needn't handle non-finite values.
Results may differ from the reference program's by a relative error of at most 0.015.
Values may be sent and summed in bfloat16 or wider, within the bound.
A program may use at most 128 MiB of HBM per device.

```python
import jax
import jax.numpy as jnp
from jax import lax

D = 2048
FF = 5632
KW = 3
SEQ_LEN = 768
TOKENS = 6144
N_TP = 4


def spiked(entries, own_key, source, target, parts, factor):
    def block_of(position):
        return (jnp.arange(entries.shape[position]) // (entries.shape[position] // parts)).reshape((-1,) + (1,) * (entries.ndim - 1 - position))

    first = jax.random.permutation(own_key, parts)[block_of(target)]
    second = (block_of(target) + parts // 2) % parts
    return jnp.where((block_of(source) == first) | (block_of(source) == second), factor * entries, entries)


def levels(rng, dims, split, low, top_value):
    level, own = 1.0, jax.random.fold_in(rng, 6)
    for axis_at, shards_of in split:
        heights = jnp.exp(jax.random.uniform(jax.random.fold_in(own, axis_at), (shards_of,), jnp.float32, low / len(split), top_value / len(split)))
        level = level * jnp.repeat(heights, dims[axis_at] // shards_of).reshape([-1 if axis == axis_at else 1 for axis in range(len(dims))])
    return level


def scatter_about(rng, shape, deviation, reach, pieces=(), held_as=jnp.bfloat16):
    factor_of = levels(rng, shape, pieces, -0.22, 0.18) if pieces else 1.0
    array = jax.random.normal(rng, shape, jnp.float32) * deviation * factor_of
    return jnp.minimum(jnp.maximum(array, -reach), reach).astype(held_as)


def gaussian_with(key, shape, spread, reach, pieces, heavy, kind=jnp.bfloat16):
    entries = spread * jax.random.normal(key, shape, jnp.float32)
    if pieces:
        entries = entries * levels(key, shape, pieces, -0.22, 0.18)
    return jnp.clip(spiked(entries, jax.random.fold_in(key, 3), *heavy), -reach, reach).astype(kind)


def setup_inputs(seed: int = 0) -> dict:
    key_of = jax.random.split(jax.random.key(seed), 10)
    return {
        "x_late": scatter_about(key_of[0], (TOKENS, D), 1.0, 6.0, ((0, 32),)),
        "x_early": scatter_about(key_of[1], (TOKENS, D), 1.0, 6.0, ((0, 32),)),
        "w_gate": scatter_about(key_of[2], (D, FF), D ** -0.5, 0.125, ((0, 8), (1, 4))),
        "w_value": scatter_about(key_of[3], (D, FF), D ** -0.5, 0.125, ((0, 8), (1, 4))),
        "conv_taps": scatter_about(key_of[4], (KW, FF), 0.6, 3.0, ((1, 4),), jnp.float32),
        "grad_hidden": gaussian_with(key_of[5], (TOKENS, FF), 1.0, 6.0, ((0, 8), (1, 4)), (0, 1, 8, 2.0)),
        "sum_gate": scatter_about(key_of[6], (D, FF), 1.0, 6.0, ((0, 8), (1, 4)), jnp.float32),
        "sum_value": scatter_about(key_of[7], (D, FF), 1.0, 6.0, ((0, 8), (1, 4)), jnp.float32),
        "sum_taps": scatter_about(key_of[8], (KW, FF), 1.0, 6.0, ((1, 4),), jnp.float32),
    }


root_half = 0.7071067811865476
density_norm = 0.3989422804014327


def causal_mix(gate_rows, taps):
    width = taps.shape[0]
    length = gate_rows.shape[0]
    padded = jnp.pad(gate_rows.astype(jnp.float32), ((width - 1, 0), (0, 0)))
    mixed_pre = jnp.zeros((length, gate_rows.shape[1]), jnp.float32)
    for j in range(width):
        mixed_pre = mixed_pre + padded[j:j + length] * taps[j]
    return mixed_pre, padded


def gelu_slope(mixed_pre):
    return 0.5 * (1.0 + lax.erf(mixed_pre * root_half)) + mixed_pre * jnp.exp(-0.5 * mixed_pre * mixed_pre) * density_norm


def back_mix(slope_rows, taps, padded):
    width = taps.shape[0]
    length = slope_rows.shape[0]
    grown = jnp.pad(slope_rows, ((0, width - 1), (0, 0)))
    d_gate = jnp.zeros(slope_rows.shape, jnp.float32)
    for j in range(width):
        d_gate = d_gate + grown[width - 1 - j:width - 1 - j + length] * taps[j]
    tap_terms = jnp.stack([jnp.sum(slope_rows * padded[j:j + length], axis=0) for j in range(width)])
    return d_gate, tap_terms


def reference(x_late, x_early, w_gate, w_value, conv_taps, grad_hidden, sum_gate, sum_value, sum_taps):
    count_seq = TOKENS // SEQ_LEN
    columns = FF // N_TP
    factor = TOKENS ** -0.5

    def project(x_rows):
        gate_rows = jnp.dot(x_rows, w_gate, preferred_element_type=jnp.float32).astype(jnp.bfloat16)
        value_rows = jnp.dot(x_rows, w_value, preferred_element_type=jnp.float32).astype(jnp.bfloat16)
        return gate_rows, value_rows

    def forward_one(x_rows):
        gate_rows, value_rows = project(x_rows)
        mixed_pre, padded = causal_mix(gate_rows, conv_taps)
        return (jax.nn.gelu(mixed_pre, approximate=False) * value_rows.astype(jnp.float32)).astype(jnp.bfloat16)

    hidden = lax.map(forward_one, x_late.reshape(count_seq, SEQ_LEN, D)).reshape(TOKENS, FF)

    def backward_one(carry, inputs):
        grad_g, grad_v, grad_t = carry
        x_rows, upstream = inputs
        gate_rows, value_rows = project(x_rows)
        mixed_pre, padded = causal_mix(gate_rows, conv_taps)
        upstream_f = upstream.astype(jnp.float32)
        slope_rows = upstream_f * value_rows.astype(jnp.float32) * gelu_slope(mixed_pre)
        d_value = (upstream_f * jax.nn.gelu(mixed_pre, approximate=False)).astype(jnp.bfloat16)
        d_gate_f, tap_terms = back_mix(slope_rows, conv_taps, padded)
        d_gate = d_gate_f.astype(jnp.bfloat16)
        grad_g = grad_g + jnp.dot(x_rows.T, d_gate, preferred_element_type=jnp.float32)
        grad_v = grad_v + jnp.dot(x_rows.T, d_value, preferred_element_type=jnp.float32)
        grad_t = grad_t + tap_terms
        total = jnp.zeros((SEQ_LEN, D), jnp.float32)
        for block in range(N_TP):
            first = block * columns
            part = jnp.dot(d_gate[:, first:first + columns], w_gate[:, first:first + columns].T, preferred_element_type=jnp.float32)
            part = part + jnp.dot(d_value[:, first:first + columns], w_value[:, first:first + columns].T, preferred_element_type=jnp.float32)
            rounded = lax.optimization_barrier(part.astype(jnp.bfloat16))
            total = total + rounded.astype(jnp.float32)
        return (grad_g, grad_v, grad_t), total.astype(jnp.bfloat16)

    start = (jnp.zeros((D, FF), jnp.float32), jnp.zeros((D, FF), jnp.float32), jnp.zeros((KW, FF), jnp.float32))
    inputs = (x_early.reshape(count_seq, SEQ_LEN, D), grad_hidden.reshape(count_seq, SEQ_LEN, FF))
    sums, grads = lax.scan(backward_one, start, inputs)
    grad_g, grad_v, grad_t = sums
    return (hidden, grads.reshape(TOKENS, D), sum_gate + factor * grad_g,
            sum_value + factor * grad_v, sum_taps + factor * grad_t)
```

```python
import math
import functools

import jax
import jax.numpy as jnp
from jax import lax
from jax.experimental import pallas as pl
from jax.experimental.pallas import tpu as pltpu
from jax.sharding import PartitionSpec as P

root_half = 0.7071067811865476
density_norm = 0.3989422804014327


def causal_mix(gate_rows, taps):
    width = taps.shape[0]
    length = gate_rows.shape[0]
    padded = jnp.pad(gate_rows.astype(jnp.float32), ((width - 1, 0), (0, 0)))
    mixed_pre = jnp.zeros((length, gate_rows.shape[1]), jnp.float32)
    for j in range(width):
        mixed_pre = mixed_pre + padded[j : j + length] * taps[j]
    return (mixed_pre, padded)


def gelu_slope(mixed_pre):
    return (
        0.5 * (1.0 + lax.erf(mixed_pre * root_half))
        + mixed_pre * jnp.exp(-0.5 * mixed_pre * mixed_pre) * density_norm
    )


def back_mix(slope_rows, taps, padded):
    width = taps.shape[0]
    length = slope_rows.shape[0]
    grown = jnp.pad(slope_rows, ((0, width - 1), (0, 0)))
    d_gate = jnp.zeros(slope_rows.shape, jnp.float32)
    for j in range(width):
        d_gate = d_gate + grown[width - 1 - j : width - 1 - j + length] * taps[j]
    tap_terms = jnp.stack(
        [jnp.sum(slope_rows * padded[j : j + length], axis=0) for j in range(width)]
    )
    return (d_gate, tap_terms)


MESH = pl.DeviceIdType.MESH


def greet(n, me):
    barrier = pltpu.get_barrier_semaphore()
    for away in range(1, n):
        pl.semaphore_signal(
            barrier, inc=1, device_id={"fs": lax.rem(me + away, n)}, device_id_type=MESH
        )
    pl.semaphore_wait(barrier, n - 1)


def gather_kernel(n, *refs):
    mine, full = refs[:2], refs[2:4]
    up_out, up_in, down_out, down_in, y_out, y_in, cross_out, cross_in, own = refs[4:]
    rows = mine[0].shape[0]
    depth = n // 2
    me = lax.axis_index("fs")
    z, y = lax.div(me, 2), lax.rem(me, 2)
    even = lax.rem(z, 2) == 0
    mate = jnp.where(even, z + 1, z - 1)

    def slot(p, zz, yy):
        return full[p].at[pl.ds(pl.multiple_of((zz * 2 + yy) * rows, rows), rows)]

    def link(p, source, zz, yy, out_sem, in_sem, to_z, to_y):
        return pltpu.make_async_remote_copy(
            src_ref=source,
            dst_ref=slot(p, zz, yy),
            send_sem=out_sem,
            recv_sem=in_sem,
            device_id={"fs": to_z * 2 + to_y},
            device_id_type=MESH,
        )

    def up(p, k):
        source = mine[p] if k == 0 else slot(p, z - k, y)
        return link(p, source, z - k, y, up_out.at[p, k], up_in.at[p, k], z + 1, y)

    def down(p, k):
        source = mine[p] if k == 0 else slot(p, z + k, y)
        return link(p, source, z + k, y, down_out.at[p, k], down_in.at[p, k], z - 1, y)

    def over(p, j, zz):
        source = mine[p] if j == 0 else slot(p, zz, y)
        return link(p, source, zz, y, y_out.at[p, j], y_in.at[p, j], z, 1 - y)

    def arrived(p, zz, yy, out_sem, in_sem):
        return link(p, slot(p, zz, yy), zz, yy, out_sem, in_sem, z, 1 - y)

    def cross():
        return link(1, slot(1, z, 1 - y), z, 1 - y, cross_out, cross_in, mate, y)

    greet(n, me)
    for p in range(2):
        pl.when(z + 1 < depth)(lambda p=p: up(p, 0).start())
        pl.when(z > 0)(lambda p=p: down(p, 0).start())
    for p in (1, 0):
        over(p, 0, z).start()
    local = [pltpu.make_async_copy(mine[p], slot(p, z, y), own.at[p]) for p in range(2)]
    for copy in local:
        copy.start()

    def y_sent(p, k, upward):
        if k == 0 and p == 1:
            return even if upward else jnp.logical_not(even)
        return None

    for k in range(depth - 1):
        for p in range(2):

            @pl.when(z - 1 - k >= 0)
            def _():
                zz = z - 1 - k
                arrived(p, zz, y, up_out.at[p, k], up_in.at[p, k]).wait_recv()
                pl.when(z + 1 < depth)(lambda: up(p, k + 1).start())
                wanted = y_sent(p, k, True)
                send = lambda: over(p, 1 + 2 * k, zz).start()
                send() if wanted is None else pl.when(wanted)(send)

            @pl.when(z + 1 + k < depth)
            def _():
                zz = z + 1 + k
                arrived(p, zz, y, down_out.at[p, k], down_in.at[p, k]).wait_recv()
                pl.when(z > 0)(lambda: down(p, k + 1).start())
                wanted = y_sent(p, k, False)
                send = lambda: over(p, 2 + 2 * k, zz).start()
                send() if wanted is None else pl.when(wanted)(send)

        if k == 0:
            arrived(1, z, 1 - y, y_out.at[1, 0], y_in.at[1, 0]).wait_recv()
            cross().start()

    arrived(0, z, 1 - y, y_out.at[0, 0], y_in.at[0, 0]).wait_recv()
    for k in range(depth - 1):
        for p in range(2):

            @pl.when(z - 1 - k >= 0)
            def _():
                wanted = y_sent(p, k, True)
                take = lambda: arrived(
                    p, z - 1 - k, 1 - y, y_out.at[p, 1 + 2 * k], y_in.at[p, 1 + 2 * k]
                ).wait_recv()
                take() if wanted is None else pl.when(wanted)(take)

            @pl.when(z + 1 + k < depth)
            def _():
                wanted = y_sent(p, k, False)
                take = lambda: arrived(
                    p, z + 1 + k, 1 - y, y_out.at[p, 2 + 2 * k], y_in.at[p, 2 + 2 * k]
                ).wait_recv()
                take() if wanted is None else pl.when(wanted)(take)

    arrived(1, mate, 1 - y, cross_out, cross_in).wait_recv()
    cross().wait_send()
    for p in range(2):
        over(p, 0, z).wait_send()
        pl.when(z + 1 < depth)(lambda p=p: up(p, 0).wait_send())
        pl.when(z > 0)(lambda p=p: down(p, 0).wait_send())
        local[p].wait()
        for k in range(depth - 1):

            @pl.when(z - 1 - k >= 0)
            def _():
                pl.when(z + 1 < depth)(lambda: up(p, k + 1).wait_send())
                wanted = y_sent(p, k, True)
                end = lambda: over(p, 1 + 2 * k, z - 1 - k).wait_send()
                end() if wanted is None else pl.when(wanted)(end)

            @pl.when(z + 1 + k < depth)
            def _():
                pl.when(z > 0)(lambda: down(p, k + 1).wait_send())
                wanted = y_sent(p, k, False)
                end = lambda: over(p, 2 + 2 * k, z + 1 + k).wait_send()
                end() if wanted is None else pl.when(wanted)(end)


def gather_rows(w_gate, w_value):
    n = lax.axis_size("fs")
    depth = n // 2
    rows, columns = w_gate.shape
    sems = pltpu.SemaphoreType.DMA
    whole = jax.ShapeDtypeStruct((n * rows, columns), w_gate.dtype)
    hbm = pl.BlockSpec(memory_space=pl.ANY)
    return pl.pallas_call(
        functools.partial(gather_kernel, n),
        out_shape=(whole, whole),
        in_specs=[hbm, hbm],
        out_specs=(hbm, hbm),
        scratch_shapes=[
            sems((2, depth)),
            sems((2, depth)),
            sems((2, depth)),
            sems((2, depth)),
            sems((2, 2 * depth)),
            sems((2, 2 * depth)),
            sems,
            sems,
            sems((2,)),
        ],
        compiler_params=pltpu.CompilerParams(collective_id=0, has_side_effects=True),
        name="gather_rows",
    )(w_gate, w_value)


def scatter_kernel(n, *refs):
    terms, taps, total, taps_total = refs[:2], refs[2], refs[3:5], refs[5]
    y_got, up_got, down_got, taps_got = refs[6:8], refs[8:10], refs[10:12], refs[12]
    y_out, y_in, z_out, up_in, down_in, taps_out, taps_in = refs[13:]
    rows = total[0].shape[0]
    depth = n // 2
    step = math.gcd(rows, 32)
    me = lax.axis_index("fs")
    z, y = lax.div(me, 2), lax.rem(me, 2)

    def start_of(zz, yy):
        return pl.multiple_of((zz * 2 + yy) * rows, rows)

    def over(p, zz):
        return pltpu.make_async_remote_copy(
            src_ref=terms[p].at[pl.ds(start_of(zz, 1 - y), rows)],
            dst_ref=y_got[p].at[zz],
            send_sem=y_out.at[p, zz],
            recv_sem=y_in.at[p, zz],
            device_id={"fs": z * 2 + 1 - y},
            device_id_type=MESH,
        )

    def along(p, zz, away, upward):
        got, sem = (up_got, up_in) if upward else (down_got, down_in)
        return pltpu.make_async_remote_copy(
            src_ref=y_got[p].at[zz],
            dst_ref=got[p].at[away - 1],
            send_sem=z_out.at[p, zz],
            recv_sem=sem.at[p, away - 1],
            device_id={"fs": (z + 1 if upward else z - 1) * 2 + y},
            device_id_type=MESH,
        )

    def taps_copy(away):
        return pltpu.make_async_remote_copy(
            src_ref=taps,
            dst_ref=taps_got.at[me],
            send_sem=taps_out.at[away],
            recv_sem=taps_in.at[me],
            device_id={"fs": lax.rem(me + away, n)},
            device_id_type=MESH,
        )

    def add(p, zz, others, into):
        base = start_of(zz, y)

        def body(i, _):
            part = pl.ds(pl.multiple_of(i * step, step), step)
            value = terms[p][
                pl.ds(pl.multiple_of(base + i * step, step), step), :
            ].astype(jnp.float32)
            value = value + y_got[p][zz, part, :].astype(jnp.float32)
            for ref, at in others:
                value = value + ref[at, part, :].astype(jnp.float32)
            if into is None:
                y_got[p][zz, part, :] = value.astype(y_got[p].dtype)
            else:
                into[part, :] = value.astype(into.dtype)
            return 0

        lax.fori_loop(0, rows // step, body, 0)

    greet(n, me)
    for away in range(depth - 1, 0, -1):
        for p in range(2):
            pl.when(z + away < depth)(lambda: over(p, z + away).start())
            pl.when(z - away >= 0)(lambda: over(p, z - away).start())
    for p in range(2):
        over(p, z).start()
    for away in range(1, n):
        taps_copy(away).start()

    def pass_on(p, away, upward):
        zz = z + away if upward else z - away
        inside = zz < depth if upward else zz >= 0
        has_more = z > 0 if upward else z + 1 < depth
        got = up_got if upward else down_got

        @pl.when(inside)
        def _():
            over(p, zz).wait_recv()

            @pl.when(has_more)
            def _():
                if away < depth - 1:
                    along(p, zz, away + 1, upward).wait_recv()
                    add(p, zz, [(got[p], away)], None)

            @pl.when(jnp.logical_not(has_more))
            def _():
                add(p, zz, [], None)

            along(p, zz, away, upward).start()

    for away in range(depth - 1, 0, -1):
        for p in range(2):
            pass_on(p, away, True)
            pass_on(p, away, False)

    taps_got[pl.ds(me, 1)] = taps[...][None]
    for away in range(1, n):
        source = lax.rem(me + away, n)
        pltpu.make_async_remote_copy(
            src_ref=taps,
            dst_ref=taps_got.at[source],
            send_sem=taps_out.at[away],
            recv_sem=taps_in.at[source],
            device_id={"fs": source},
            device_id_type=MESH,
        ).wait_recv()
    sum_of = taps_got[0]
    for i in range(1, n):
        sum_of = sum_of + taps_got[i]
    taps_total[...] = sum_of

    for p in range(2):
        over(p, z).wait_recv()
        pl.when(z > 0)(lambda: along(p, z, 1, True).wait_recv())
        pl.when(z + 1 < depth)(lambda: along(p, z, 1, False).wait_recv())
        at_low, at_high = z == 0, z + 1 == depth
        both = jnp.logical_not(jnp.logical_or(at_low, at_high))
        pl.when(at_low)(lambda: add(p, z, [(down_got[p], 0)], total[p]))
        pl.when(at_high)(lambda: add(p, z, [(up_got[p], 0)], total[p]))
        pl.when(both)(lambda: add(p, z, [(up_got[p], 0), (down_got[p], 0)], total[p]))

    for p in range(2):
        over(p, z).wait_send()
        for away in range(depth - 1, 0, -1):

            @pl.when(z + away < depth)
            def _():
                over(p, z + away).wait_send()
                along(p, z + away, away, True).wait_send()

            @pl.when(z - away >= 0)
            def _():
                over(p, z - away).wait_send()
                along(p, z - away, away, False).wait_send()

    for away in range(1, n):
        taps_copy(away).wait_send()


def scatter_rows(gate_terms, value_terms, tap_terms):
    n = lax.axis_size("fs")
    depth = n // 2
    rows, columns = gate_terms.shape[0] // n, gate_terms.shape[1]
    sems = pltpu.SemaphoreType.DMA
    vmem = pl.BlockSpec(memory_space=pltpu.VMEM)
    total = jax.ShapeDtypeStruct((rows, columns), jnp.float32)
    row_block = lambda count: pltpu.VMEM((count, rows, columns), gate_terms.dtype)
    return pl.pallas_call(
        functools.partial(scatter_kernel, n),
        out_shape=(total, total, jax.ShapeDtypeStruct(tap_terms.shape, jnp.float32)),
        in_specs=[vmem] * 3,
        out_specs=(vmem,) * 3,
        scratch_shapes=[row_block(depth)] * 2
        + [row_block(depth - 1)] * 4
        + [
            pltpu.VMEM((n,) + tap_terms.shape, jnp.float32),
            sems((2, depth)),
            sems((2, depth)),
            sems((2, depth)),
            sems((2, depth)),
            sems((2, depth)),
            sems((n,)),
            sems((n,)),
        ],
        compiler_params=pltpu.CompilerParams(
            collective_id=1, has_side_effects=True, vmem_limit_bytes=60 * 1024 * 1024
        ),
        name="scatter_rows",
    )(gate_terms, value_terms, tap_terms)


def shards(x_late, x_early, w_gate, w_value, conv_taps, grad_hidden, sum_gate, sum_value, sum_taps):
    columns = w_gate.shape[1]
    factor = 1.0 / math.sqrt(x_late.shape[0] * lax.axis_size("fs") * lax.axis_size("tp"))
    gate_full, value_full = gather_rows(w_gate, w_value)
    block_rows = lax.all_gather(x_late, "tp", axis=0, tiled=True)
    gate_part = jnp.dot(block_rows, gate_full, preferred_element_type=jnp.float32).astype(
        jnp.bfloat16
    )
    value_part = jnp.dot(block_rows, value_full, preferred_element_type=jnp.float32).astype(
        jnp.bfloat16
    )
    projected = jnp.concatenate([gate_part, value_part], axis=1)
    gate_rows = projected[:, :columns]
    value_rows = projected[:, columns:]
    mixed_pre, padded = causal_mix(gate_rows, conv_taps)
    hidden = (jax.nn.gelu(mixed_pre, approximate=False) * value_rows.astype(jnp.float32)).astype(
        jnp.bfloat16
    )
    gathered = lax.all_gather(x_early, "tp", axis=0, tiled=True)
    gate_rows = jnp.dot(gathered, gate_full, preferred_element_type=jnp.float32).astype(
        jnp.bfloat16
    )
    value_rows = jnp.dot(gathered, value_full, preferred_element_type=jnp.float32).astype(
        jnp.bfloat16
    )
    mixed_pre, padded = causal_mix(gate_rows, conv_taps)
    upstream = grad_hidden.astype(jnp.float32)
    slope_rows = upstream * value_rows.astype(jnp.float32) * gelu_slope(mixed_pre)
    d_gate_f, tap_terms = back_mix(slope_rows, conv_taps, padded)
    d_gate = d_gate_f.astype(jnp.bfloat16)
    d_value = (upstream * jax.nn.gelu(mixed_pre, approximate=False)).astype(jnp.bfloat16)
    contract = (((1,), (1,)), ((), ()))
    grad_early = lax.psum_scatter(
        (
            lax.dot_general(d_gate, gate_full, contract, preferred_element_type=jnp.float32)
            + lax.dot_general(d_value, value_full, contract, preferred_element_type=jnp.float32)
        ).astype(jnp.bfloat16),
        "tp",
        scatter_dimension=0,
        tiled=True,
    )
    outer = (((0,), (0,)), ((), ()))
    gate_terms = lax.dot_general(gathered, d_gate, outer, preferred_element_type=jnp.float32)
    value_terms = lax.dot_general(gathered, d_value, outer, preferred_element_type=jnp.float32)
    taps_padded = jnp.pad(factor * tap_terms, ((0, -tap_terms.shape[0] % 8), (0, 0)))
    gate_total, value_total, tap_total = scatter_rows(
        (factor * gate_terms).astype(jnp.bfloat16),
        (factor * value_terms).astype(jnp.bfloat16),
        taps_padded,
    )
    tap_total = tap_total[: tap_terms.shape[0]]
    return (
        hidden,
        grad_early,
        sum_gate + gate_total,
        sum_value + value_total,
        sum_taps + tap_total,
    )


def solution(mesh):
    placed = (
        P(("fs", "tp"), None),
        P(("fs", "tp"), None),
        P("fs", "tp"),
        P("fs", "tp"),
        P(None, "tp"),
        P("fs", "tp"),
        P("fs", "tp"),
        P("fs", "tp"),
        P(None, "tp"),
    )
    return jax.shard_map(
        shards,
        mesh=mesh,
        in_specs=placed,
        out_specs=(
            P("fs", "tp"),
            P(("fs", "tp"), None),
            P("fs", "tp"),
            P("fs", "tp"),
            P(None, "tp"),
        ),
        check_vma=False,
    )
```

```python
import math
import functools

import jax
import jax.numpy as jnp
from jax import lax
from jax.experimental import pallas as pl
from jax.experimental.pallas import tpu as pltpu
from jax.sharding import PartitionSpec as P

root_half = 0.7071067811865476
density_norm = 0.3989422804014327


def causal_mix(gate_rows, taps):
    width = taps.shape[0]
    length = gate_rows.shape[0]
    padded = jnp.pad(gate_rows.astype(jnp.float32), ((width - 1, 0), (0, 0)))
    mixed_pre = jnp.zeros((length, gate_rows.shape[1]), jnp.float32)
    for j in range(width):
        mixed_pre = mixed_pre + padded[j : j + length] * taps[j]
    return (mixed_pre, padded)


def gelu_slope(mixed_pre):
    return (
        0.5 * (1.0 + lax.erf(mixed_pre * root_half))
        + mixed_pre * jnp.exp(-0.5 * mixed_pre * mixed_pre) * density_norm
    )


def back_mix(slope_rows, taps, padded):
    width = taps.shape[0]
    length = slope_rows.shape[0]
    grown = jnp.pad(slope_rows, ((0, width - 1), (0, 0)))
    d_gate = jnp.zeros(slope_rows.shape, jnp.float32)
    for j in range(width):
        d_gate = d_gate + grown[width - 1 - j : width - 1 - j + length] * taps[j]
    tap_terms = jnp.stack(
        [jnp.sum(slope_rows * padded[j : j + length], axis=0) for j in range(width)]
    )
    return (d_gate, tap_terms)


MESH = pl.DeviceIdType.MESH


def greet(n, me):
    barrier = pltpu.get_barrier_semaphore()
    for away in range(1, n):
        pl.semaphore_signal(
            barrier, inc=1, device_id={"fs": lax.rem(me + away, n)}, device_id_type=MESH
        )
    pl.semaphore_wait(barrier, n - 1)


def gather_kernel(n, *refs):
    mine, full = refs[:2], refs[2:4]
    up_out, up_in, down_out, down_in, y_out, y_in, cross_out, cross_in, own = refs[4:]
    rows = mine[0].shape[0]
    depth = n // 2
    me = lax.axis_index("fs")
    z, y = lax.div(me, 2), lax.rem(me, 2)
    even = lax.rem(z, 2) == 0
    mate = jnp.where(even, z + 1, z - 1)

    def slot(p, zz, yy):
        return full[p].at[pl.ds(pl.multiple_of((zz * 2 + yy) * rows, rows), rows)]

    def link(p, source, zz, yy, out_sem, in_sem, to_z, to_y):
        return pltpu.make_async_remote_copy(
            src_ref=source,
            dst_ref=slot(p, zz, yy),
            send_sem=out_sem,
            recv_sem=in_sem,
            device_id={"fs": to_z * 2 + to_y},
            device_id_type=MESH,
        )

    def up(p, k):
        source = mine[p] if k == 0 else slot(p, z - k, y)
        return link(p, source, z - k, y, up_out.at[p, k], up_in.at[p, k], z + 1, y)

    def down(p, k):
        source = mine[p] if k == 0 else slot(p, z + k, y)
        return link(p, source, z + k, y, down_out.at[p, k], down_in.at[p, k], z - 1, y)

    def over(p, j, zz):
        source = mine[p] if j == 0 else slot(p, zz, y)
        return link(p, source, zz, y, y_out.at[p, j], y_in.at[p, j], z, 1 - y)

    def arrived(p, zz, yy, out_sem, in_sem):
        return link(p, slot(p, zz, yy), zz, yy, out_sem, in_sem, z, 1 - y)

    def cross():
        return link(1, slot(1, z, 1 - y), z, 1 - y, cross_out, cross_in, mate, y)

    greet(n, me)
    for p in range(2):
        pl.when(z + 1 < depth)(lambda p=p: up(p, 0).start())
        pl.when(z > 0)(lambda p=p: down(p, 0).start())
    for p in (1, 0):
        over(p, 0, z).start()
    local = [pltpu.make_async_copy(mine[p], slot(p, z, y), own.at[p]) for p in range(2)]
    for copy in local:
        copy.start()

    def y_sent(p, k, upward):
        if k == 0 and p == 1:
            return even if upward else jnp.logical_not(even)
        return None

    for k in range(depth - 1):
        for p in range(2):

            @pl.when(z - 1 - k >= 0)
            def _():
                zz = z - 1 - k
                arrived(p, zz, y, up_out.at[p, k], up_in.at[p, k]).wait_recv()
                pl.when(z + 1 < depth)(lambda: up(p, k + 1).start())
                wanted = y_sent(p, k, True)
                send = lambda: over(p, 1 + 2 * k, zz).start()
                send() if wanted is None else pl.when(wanted)(send)

            @pl.when(z + 1 + k < depth)
            def _():
                zz = z + 1 + k
                arrived(p, zz, y, down_out.at[p, k], down_in.at[p, k]).wait_recv()
                pl.when(z > 0)(lambda: down(p, k + 1).start())
                wanted = y_sent(p, k, False)
                send = lambda: over(p, 2 + 2 * k, zz).start()
                send() if wanted is None else pl.when(wanted)(send)

        if k == 0:
            arrived(1, z, 1 - y, y_out.at[1, 0], y_in.at[1, 0]).wait_recv()
            cross().start()

    arrived(0, z, 1 - y, y_out.at[0, 0], y_in.at[0, 0]).wait_recv()
    for k in range(depth - 1):
        for p in range(2):

            @pl.when(z - 1 - k >= 0)
            def _():
                wanted = y_sent(p, k, True)
                take = lambda: arrived(
                    p, z - 1 - k, 1 - y, y_out.at[p, 1 + 2 * k], y_in.at[p, 1 + 2 * k]
                ).wait_recv()
                take() if wanted is None else pl.when(wanted)(take)

            @pl.when(z + 1 + k < depth)
            def _():
                wanted = y_sent(p, k, False)
                take = lambda: arrived(
                    p, z + 1 + k, 1 - y, y_out.at[p, 2 + 2 * k], y_in.at[p, 2 + 2 * k]
                ).wait_recv()
                take() if wanted is None else pl.when(wanted)(take)

    arrived(1, mate, 1 - y, cross_out, cross_in).wait_recv()
    cross().wait_send()
    for p in range(2):
        over(p, 0, z).wait_send()
        pl.when(z + 1 < depth)(lambda p=p: up(p, 0).wait_send())
        pl.when(z > 0)(lambda p=p: down(p, 0).wait_send())
        local[p].wait()
        for k in range(depth - 1):

            @pl.when(z - 1 - k >= 0)
            def _():
                pl.when(z + 1 < depth)(lambda: up(p, k + 1).wait_send())
                wanted = y_sent(p, k, True)
                end = lambda: over(p, 1 + 2 * k, z - 1 - k).wait_send()
                end() if wanted is None else pl.when(wanted)(end)

            @pl.when(z + 1 + k < depth)
            def _():
                pl.when(z > 0)(lambda: down(p, k + 1).wait_send())
                wanted = y_sent(p, k, False)
                end = lambda: over(p, 2 + 2 * k, z + 1 + k).wait_send()
                end() if wanted is None else pl.when(wanted)(end)


def gather_rows(w_gate, w_value):
    n = lax.axis_size("fs")
    depth = n // 2
    rows, columns = w_gate.shape
    sems = pltpu.SemaphoreType.DMA
    whole = jax.ShapeDtypeStruct((n * rows, columns), w_gate.dtype)
    hbm = pl.BlockSpec(memory_space=pl.ANY)
    return pl.pallas_call(
        functools.partial(gather_kernel, n),
        out_shape=(whole, whole),
        in_specs=[hbm, hbm],
        out_specs=(hbm, hbm),
        scratch_shapes=[
            sems((2, depth)),
            sems((2, depth)),
            sems((2, depth)),
            sems((2, depth)),
            sems((2, 2 * depth)),
            sems((2, 2 * depth)),
            sems,
            sems,
            sems((2,)),
        ],
        compiler_params=pltpu.CompilerParams(collective_id=0, has_side_effects=True),
        name="gather_rows",
    )(w_gate, w_value)


def scatter_kernel(n, *refs):
    terms, taps, rows_late, weights, conv = refs[:2], refs[2], refs[3], refs[4:6], refs[6]
    total, taps_total, hidden = refs[7:9], refs[9], refs[10]
    y_got, up_got, down_got, taps_got = refs[11:13], refs[13:15], refs[15:17], refs[17]
    cross_got, strip = refs[18], refs[19]
    y_out, y_in, z_out, up_in, down_in, taps_out, taps_in = refs[20:27]
    cross_out, cross_in, strip_in = refs[27:]
    rows = total[0].shape[0]
    depth = n // 2
    step = math.gcd(rows, 32)
    me = lax.axis_index("fs")
    z, y = lax.div(me, 2), lax.rem(me, 2)
    even = lax.rem(z, 2) == 0
    odd = jnp.logical_not(even)
    mate = jnp.where(even, z + 1, z - 1)
    lane = 128
    strips = hidden.shape[1] // lane

    def fetch(b):
        at = pl.ds(pl.multiple_of(b * lane, lane), lane)
        slot = lax.rem(b, 2)
        return [
            pltpu.make_async_copy(
                weights[i].at[:, at],
                strip.at[slot, :, pl.ds(i * lane, lane)],
                strip_in.at[slot, i],
            )
            for i in range(2)
        ]

    def late(first, last):
        def body(b, _):
            for copy in fetch(b):
                copy.wait()

            @pl.when(b + 1 < strips)
            def _():
                for copy in fetch(b + 1):
                    copy.start()

            at = pl.ds(pl.multiple_of(b * lane, lane), lane)
            both = jnp.dot(
                rows_late[...], strip[lax.rem(b, 2)], preferred_element_type=jnp.float32
            )
            both = both.astype(jnp.bfloat16).astype(jnp.float32)
            gate = both[:, :lane]
            width = conv.shape[0]
            position = lax.broadcasted_iota(jnp.int32, gate.shape, 0)
            pre = gate * conv[pl.ds(width - 1, 1), at]
            for j in range(width - 1):
                lag = width - 1 - j
                moved = jnp.where(position >= lag, pltpu.roll(gate, lag, 0), 0.0)
                pre = pre + moved * conv[pl.ds(j, 1), at]
            active = 0.5 * pre * (1.0 + lax.erf(pre * root_half))
            hidden[:, at] = (active * both[:, lane:]).astype(hidden.dtype)
            return 0

        lax.fori_loop(first, last, body, 0)

    def start_of(zz, yy):
        return pl.multiple_of((zz * 2 + yy) * rows, rows)

    def over(p, zz, source=None):
        return pltpu.make_async_remote_copy(
            src_ref=terms[p].at[pl.ds(start_of(zz, 1 - y), rows)] if source is None else source,
            dst_ref=y_got[p].at[zz],
            send_sem=y_out.at[p, zz],
            recv_sem=y_in.at[p, zz],
            device_id={"fs": z * 2 + 1 - y},
            device_id_type=MESH,
        )

    def along(p, zz, away, upward):
        got, sem = (up_got, up_in) if upward else (down_got, down_in)
        return pltpu.make_async_remote_copy(
            src_ref=y_got[p].at[zz],
            dst_ref=got[p].at[away - 1],
            send_sem=z_out.at[p, zz],
            recv_sem=sem.at[p, away - 1],
            device_id={"fs": (z + 1 if upward else z - 1) * 2 + y},
            device_id_type=MESH,
        )

    def cross():
        return pltpu.make_async_remote_copy(
            src_ref=terms[1].at[pl.ds(start_of(mate, 1 - y), rows)],
            dst_ref=cross_got,
            send_sem=cross_out,
            recv_sem=cross_in,
            device_id={"fs": mate * 2 + y},
            device_id_type=MESH,
        )

    def add_cross():
        base = start_of(z, 1 - y)

        def body(i, _):
            part = pl.ds(pl.multiple_of(i * step, step), step)
            value = terms[1][pl.ds(pl.multiple_of(base + i * step, step), step), :]
            value = value.astype(jnp.float32) + cross_got[part, :].astype(jnp.float32)
            cross_got[part, :] = value.astype(cross_got.dtype)
            return 0

        lax.fori_loop(0, rows // step, body, 0)

    def over_y(p, away, upward):
        if p == 1 and away == 1:
            return odd if upward else even
        return True

    def taps_copy(away):
        return pltpu.make_async_remote_copy(
            src_ref=taps,
            dst_ref=taps_got.at[me],
            send_sem=taps_out.at[away],
            recv_sem=taps_in.at[me],
            device_id={"fs": lax.rem(me + away, n)},
            device_id_type=MESH,
        )

    def add(p, zz, others, into, from_y=True):
        base = start_of(zz, y)

        def body(i, _):
            part = pl.ds(pl.multiple_of(i * step, step), step)
            value = terms[p][
                pl.ds(pl.multiple_of(base + i * step, step), step), :
            ].astype(jnp.float32)
            if from_y:
                value = value + y_got[p][zz, part, :].astype(jnp.float32)
            for ref, at in others:
                value = value + ref[at, part, :].astype(jnp.float32)
            if into is None:
                y_got[p][zz, part, :] = value.astype(y_got[p].dtype)
            else:
                into[part, :] = value.astype(into.dtype)
            return 0

        lax.fori_loop(0, rows // step, body, 0)

    for copy in fetch(0):
        copy.start()
    greet(n, me)
    cross().start()
    for away in range(depth - 1, 0, -1):
        for p in range(2):
            up_too, down_too = over_y(p, away, True), over_y(p, away, False)
            pl.when(jnp.logical_and(z + away < depth, up_too))(
                lambda: over(p, z + away).start()
            )
            pl.when(jnp.logical_and(z - away >= 0, down_too))(
                lambda: over(p, z - away).start()
            )
    over(0, z).start()
    for away in range(1, n):
        taps_copy(away).start()

    def pass_on(p, away, upward):
        zz = z + away if upward else z - away
        inside = zz < depth if upward else zz >= 0
        has_more = z > 0 if upward else z + 1 < depth
        got = up_got if upward else down_got
        kinds = [(True, True)]
        if p == 1 and away == 1:
            kinds = [(True, odd if upward else even), (False, even if upward else odd)]

        @pl.when(inside)
        def _():
            if away < depth - 1:
                pl.when(has_more)(lambda: along(p, zz, away + 1, upward).wait_recv())
            for from_y, here in kinds:

                @pl.when(jnp.logical_and(inside, here))
                def _():
                    if from_y:
                        over(p, zz).wait_recv()

                    @pl.when(has_more)
                    def _():
                        add(p, zz, [(got[p], away)] if away < depth - 1 else [], None, from_y)

                    @pl.when(jnp.logical_not(has_more))
                    def _():
                        add(p, zz, [], None, from_y)

            along(p, zz, away, upward).start()

    done = min(4, strips)
    late(0, done)
    for away in range(depth - 1, 0, -1):
        for p in range(2):
            pass_on(p, away, True)
            pass_on(p, away, False)
            if away == depth - 1 and p == 1:
                cross().wait_recv()
                add_cross()
                over(1, z, cross_got).start()
            if done < strips:
                upto = min(done + 2, strips)
                late(done, upto)
                done = upto
    if done < strips:
        late(done, strips)

    taps_got[pl.ds(me, 1)] = taps[...][None]
    for away in range(1, n):
        source = lax.rem(me + away, n)
        pltpu.make_async_remote_copy(
            src_ref=taps,
            dst_ref=taps_got.at[source],
            send_sem=taps_out.at[away],
            recv_sem=taps_in.at[source],
            device_id={"fs": source},
            device_id_type=MESH,
        ).wait_recv()
    sum_of = taps_got[0]
    for i in range(1, n):
        sum_of = sum_of + taps_got[i]
    taps_total[...] = sum_of

    for p in range(2):
        over(p, z).wait_recv()
        pl.when(z > 0)(lambda: along(p, z, 1, True).wait_recv())
        pl.when(z + 1 < depth)(lambda: along(p, z, 1, False).wait_recv())
        at_low, at_high = z == 0, z + 1 == depth
        both = jnp.logical_not(jnp.logical_or(at_low, at_high))
        pl.when(at_low)(lambda: add(p, z, [(down_got[p], 0)], total[p]))
        pl.when(at_high)(lambda: add(p, z, [(up_got[p], 0)], total[p]))
        pl.when(both)(lambda: add(p, z, [(up_got[p], 0), (down_got[p], 0)], total[p]))

    cross().wait_send()
    over(0, z).wait_send()
    over(1, z, cross_got).wait_send()
    for p in range(2):
        for away in range(depth - 1, 0, -1):
            up_too, down_too = over_y(p, away, True), over_y(p, away, False)

            @pl.when(z + away < depth)
            def _():
                pl.when(jnp.logical_and(z + away < depth, up_too))(
                    lambda: over(p, z + away).wait_send()
                )
                along(p, z + away, away, True).wait_send()

            @pl.when(z - away >= 0)
            def _():
                pl.when(jnp.logical_and(z - away >= 0, down_too))(
                    lambda: over(p, z - away).wait_send()
                )
                along(p, z - away, away, False).wait_send()

    for away in range(1, n):
        taps_copy(away).wait_send()


def scatter_rows(gate_terms, value_terms, tap_terms, rows_late, gate_full, value_full, conv_taps):
    n = lax.axis_size("fs")
    depth = n // 2
    rows, columns = gate_terms.shape[0] // n, gate_terms.shape[1]
    sems = pltpu.SemaphoreType.DMA
    vmem = pl.BlockSpec(memory_space=pltpu.VMEM)
    total = jax.ShapeDtypeStruct((rows, columns), jnp.float32)
    row_block = lambda count: pltpu.VMEM((count, rows, columns), gate_terms.dtype)
    return pl.pallas_call(
        functools.partial(scatter_kernel, n),
        out_shape=(
            total,
            total,
            jax.ShapeDtypeStruct(tap_terms.shape, jnp.float32),
            jax.ShapeDtypeStruct((rows_late.shape[0], columns), jnp.bfloat16),
        ),
        in_specs=[vmem] * 4 + [pl.BlockSpec(memory_space=pl.ANY)] * 2 + [vmem],
        out_specs=(vmem,) * 4,
        scratch_shapes=[row_block(depth)] * 2
        + [row_block(depth - 1)] * 4
        + [
            pltpu.VMEM((n,) + tap_terms.shape, jnp.float32),
            pltpu.VMEM((rows, columns), gate_terms.dtype),
            pltpu.VMEM((2, gate_full.shape[0], 256), gate_full.dtype),
            sems((2, depth)),
            sems((2, depth)),
            sems((2, depth)),
            sems((2, depth)),
            sems((2, depth)),
            sems((n,)),
            sems((n,)),
            sems,
            sems,
            sems((2, 2)),
        ],
        compiler_params=pltpu.CompilerParams(
            collective_id=1, has_side_effects=True, vmem_limit_bytes=60 * 1024 * 1024
        ),
        name="scatter_rows",
    )(gate_terms, value_terms, tap_terms, rows_late, gate_full, value_full, conv_taps)


def shards(x_late, x_early, w_gate, w_value, conv_taps, grad_hidden, sum_gate, sum_value, sum_taps):
    columns = w_gate.shape[1]
    factor = 1.0 / math.sqrt(x_late.shape[0] * lax.axis_size("fs") * lax.axis_size("tp"))
    gate_full, value_full = gather_rows(w_gate, w_value)
    block_rows = lax.all_gather(x_late, "tp", axis=0, tiled=True)
    gathered = lax.all_gather(x_early, "tp", axis=0, tiled=True)
    gate_rows = jnp.dot(gathered, gate_full, preferred_element_type=jnp.float32).astype(
        jnp.bfloat16
    )
    value_rows = jnp.dot(gathered, value_full, preferred_element_type=jnp.float32).astype(
        jnp.bfloat16
    )
    mixed_pre, padded = causal_mix(gate_rows, conv_taps)
    upstream = grad_hidden.astype(jnp.float32)
    slope_rows = upstream * value_rows.astype(jnp.float32) * gelu_slope(mixed_pre)
    d_gate_f, tap_terms = back_mix(slope_rows, conv_taps, padded)
    d_gate = d_gate_f.astype(jnp.bfloat16)
    d_value = (upstream * jax.nn.gelu(mixed_pre, approximate=False)).astype(jnp.bfloat16)
    contract = (((1,), (1,)), ((), ()))
    grad_early = lax.psum_scatter(
        (
            lax.dot_general(d_gate, gate_full, contract, preferred_element_type=jnp.float32)
            + lax.dot_general(d_value, value_full, contract, preferred_element_type=jnp.float32)
        ).astype(jnp.bfloat16),
        "tp",
        scatter_dimension=0,
        tiled=True,
    )
    outer = (((0,), (0,)), ((), ()))
    gate_terms = lax.dot_general(gathered, d_gate, outer, preferred_element_type=jnp.float32)
    value_terms = lax.dot_general(gathered, d_value, outer, preferred_element_type=jnp.float32)
    taps_padded = jnp.pad(factor * tap_terms, ((0, -tap_terms.shape[0] % 8), (0, 0)))
    gate_total, value_total, tap_total, hidden = scatter_rows(
        (factor * gate_terms).astype(jnp.bfloat16),
        (factor * value_terms).astype(jnp.bfloat16),
        taps_padded,
        block_rows,
        gate_full,
        value_full,
        conv_taps,
    )
    tap_total = tap_total[: tap_terms.shape[0]]
    return (
        hidden,
        grad_early,
        sum_gate + gate_total,
        sum_value + value_total,
        sum_taps + tap_total,
    )


def solution(mesh):
    placed = (
        P(("fs", "tp"), None),
        P(("fs", "tp"), None),
        P("fs", "tp"),
        P("fs", "tp"),
        P(None, "tp"),
        P("fs", "tp"),
        P("fs", "tp"),
        P("fs", "tp"),
        P(None, "tp"),
    )
    return jax.shard_map(
        shards,
        mesh=mesh,
        in_specs=placed,
        out_specs=(
            P("fs", "tp"),
            P(("fs", "tp"), None),
            P("fs", "tp"),
            P("fs", "tp"),
            P(None, "tp"),
        ),
        check_vma=False,
    )
```

```python
import math
import functools

import jax
import jax.numpy as jnp
from jax import lax
from jax.experimental import pallas as pl
from jax.experimental.pallas import tpu as pltpu
from jax.sharding import PartitionSpec as P

root_half = 0.7071067811865476
density_norm = 0.3989422804014327


def causal_mix(gate_rows, taps):
    width = taps.shape[0]
    length = gate_rows.shape[0]
    padded = jnp.pad(gate_rows.astype(jnp.float32), ((width - 1, 0), (0, 0)))
    mixed_pre = jnp.zeros((length, gate_rows.shape[1]), jnp.float32)
    for j in range(width):
        mixed_pre = mixed_pre + padded[j : j + length] * taps[j]
    return (mixed_pre, padded)


def gelu_slope(mixed_pre):
    return (
        0.5 * (1.0 + lax.erf(mixed_pre * root_half))
        + mixed_pre * jnp.exp(-0.5 * mixed_pre * mixed_pre) * density_norm
    )


def back_mix(slope_rows, taps, padded):
    width = taps.shape[0]
    length = slope_rows.shape[0]
    grown = jnp.pad(slope_rows, ((0, width - 1), (0, 0)))
    d_gate = jnp.zeros(slope_rows.shape, jnp.float32)
    for j in range(width):
        d_gate = d_gate + grown[width - 1 - j : width - 1 - j + length] * taps[j]
    tap_terms = jnp.stack(
        [jnp.sum(slope_rows * padded[j : j + length], axis=0) for j in range(width)]
    )
    return (d_gate, tap_terms)


MESH = pl.DeviceIdType.MESH


def greet(n, me):
    barrier = pltpu.get_barrier_semaphore()
    for away in range(1, n):
        pl.semaphore_signal(
            barrier, inc=1, device_id={"fs": lax.rem(me + away, n)}, device_id_type=MESH
        )
    pl.semaphore_wait(barrier, n - 1)


def gather_kernel(n, *refs):
    mine, full = refs[:2], refs[2:4]
    up_out, up_in, down_out, down_in, y_out, y_in, cross_out, cross_in, own = refs[4:]
    rows = mine[0].shape[0]
    depth = n // 2
    me = lax.axis_index("fs")
    z, y = lax.div(me, 2), lax.rem(me, 2)
    even = lax.rem(z, 2) == 0
    mate = jnp.where(even, z + 1, z - 1)

    def slot(p, zz, yy):
        return full[p].at[pl.ds(pl.multiple_of((zz * 2 + yy) * rows, rows), rows)]

    def link(p, source, zz, yy, out_sem, in_sem, to_z, to_y):
        return pltpu.make_async_remote_copy(
            src_ref=source,
            dst_ref=slot(p, zz, yy),
            send_sem=out_sem,
            recv_sem=in_sem,
            device_id={"fs": to_z * 2 + to_y},
            device_id_type=MESH,
        )

    def up(p, k):
        source = mine[p] if k == 0 else slot(p, z - k, y)
        return link(p, source, z - k, y, up_out.at[p, k], up_in.at[p, k], z + 1, y)

    def down(p, k):
        source = mine[p] if k == 0 else slot(p, z + k, y)
        return link(p, source, z + k, y, down_out.at[p, k], down_in.at[p, k], z - 1, y)

    def over(p, j, zz):
        source = mine[p] if j == 0 else slot(p, zz, y)
        return link(p, source, zz, y, y_out.at[p, j], y_in.at[p, j], z, 1 - y)

    def arrived(p, zz, yy, out_sem, in_sem):
        return link(p, slot(p, zz, yy), zz, yy, out_sem, in_sem, z, 1 - y)

    def cross():
        return link(1, slot(1, z, 1 - y), z, 1 - y, cross_out, cross_in, mate, y)

    greet(n, me)
    for p in range(2):
        pl.when(z + 1 < depth)(lambda p=p: up(p, 0).start())
        pl.when(z > 0)(lambda p=p: down(p, 0).start())
    for p in (1, 0):
        over(p, 0, z).start()
    local = [pltpu.make_async_copy(mine[p], slot(p, z, y), own.at[p]) for p in range(2)]
    for copy in local:
        copy.start()

    def y_sent(p, k, upward):
        if k == 0 and p == 1:
            return even if upward else jnp.logical_not(even)
        return None

    for k in range(depth - 1):
        for p in range(2):

            @pl.when(z - 1 - k >= 0)
            def _():
                zz = z - 1 - k
                arrived(p, zz, y, up_out.at[p, k], up_in.at[p, k]).wait_recv()
                pl.when(z + 1 < depth)(lambda: up(p, k + 1).start())
                wanted = y_sent(p, k, True)
                send = lambda: over(p, 1 + 2 * k, zz).start()
                send() if wanted is None else pl.when(wanted)(send)

            @pl.when(z + 1 + k < depth)
            def _():
                zz = z + 1 + k
                arrived(p, zz, y, down_out.at[p, k], down_in.at[p, k]).wait_recv()
                pl.when(z > 0)(lambda: down(p, k + 1).start())
                wanted = y_sent(p, k, False)
                send = lambda: over(p, 2 + 2 * k, zz).start()
                send() if wanted is None else pl.when(wanted)(send)

        if k == 0:
            arrived(1, z, 1 - y, y_out.at[1, 0], y_in.at[1, 0]).wait_recv()
            cross().start()

    arrived(0, z, 1 - y, y_out.at[0, 0], y_in.at[0, 0]).wait_recv()
    for k in range(depth - 1):
        for p in range(2):

            @pl.when(z - 1 - k >= 0)
            def _():
                wanted = y_sent(p, k, True)
                take = lambda: arrived(
                    p, z - 1 - k, 1 - y, y_out.at[p, 1 + 2 * k], y_in.at[p, 1 + 2 * k]
                ).wait_recv()
                take() if wanted is None else pl.when(wanted)(take)

            @pl.when(z + 1 + k < depth)
            def _():
                wanted = y_sent(p, k, False)
                take = lambda: arrived(
                    p, z + 1 + k, 1 - y, y_out.at[p, 2 + 2 * k], y_in.at[p, 2 + 2 * k]
                ).wait_recv()
                take() if wanted is None else pl.when(wanted)(take)

    arrived(1, mate, 1 - y, cross_out, cross_in).wait_recv()
    cross().wait_send()
    for p in range(2):
        over(p, 0, z).wait_send()
        pl.when(z + 1 < depth)(lambda p=p: up(p, 0).wait_send())
        pl.when(z > 0)(lambda p=p: down(p, 0).wait_send())
        local[p].wait()
        for k in range(depth - 1):

            @pl.when(z - 1 - k >= 0)
            def _():
                pl.when(z + 1 < depth)(lambda: up(p, k + 1).wait_send())
                wanted = y_sent(p, k, True)
                end = lambda: over(p, 1 + 2 * k, z - 1 - k).wait_send()
                end() if wanted is None else pl.when(wanted)(end)

            @pl.when(z + 1 + k < depth)
            def _():
                pl.when(z > 0)(lambda: down(p, k + 1).wait_send())
                wanted = y_sent(p, k, False)
                end = lambda: over(p, 2 + 2 * k, z + 1 + k).wait_send()
                end() if wanted is None else pl.when(wanted)(end)


def gather_rows(w_gate, w_value):
    n = lax.axis_size("fs")
    depth = n // 2
    rows, columns = w_gate.shape
    sems = pltpu.SemaphoreType.DMA
    whole = jax.ShapeDtypeStruct((n * rows, columns), w_gate.dtype)
    hbm = pl.BlockSpec(memory_space=pl.ANY)
    return pl.pallas_call(
        functools.partial(gather_kernel, n),
        out_shape=(whole, whole),
        in_specs=[hbm, hbm],
        out_specs=(hbm, hbm),
        scratch_shapes=[
            sems((2, depth)),
            sems((2, depth)),
            sems((2, depth)),
            sems((2, depth)),
            sems((2, 2 * depth)),
            sems((2, 2 * depth)),
            sems,
            sems,
            sems((2,)),
        ],
        compiler_params=pltpu.CompilerParams(collective_id=0, has_side_effects=True),
        name="gather_rows",
    )(w_gate, w_value)


def scatter_kernel(n, factor, *refs):
    flipped, deltas, taps, rows_late = refs[0], refs[1:3], refs[3], refs[4]
    weights, conv = refs[5:7], refs[7]
    total, taps_total, hidden = refs[8:10], refs[10], refs[11]
    y_got, up_got, down_got, taps_got = refs[12:14], refs[14:16], refs[16:18], refs[18]
    cross_got, strip, terms = refs[19], refs[20], refs[21:23]
    y_out, y_in, z_out, up_in, down_in, taps_out, taps_in = refs[23:30]
    cross_out, cross_in, strip_in = refs[30:]
    rows = total[0].shape[0]
    depth = n // 2
    step = math.gcd(rows, 32)
    me = lax.axis_index("fs")
    z, y = lax.div(me, 2), lax.rem(me, 2)
    even = lax.rem(z, 2) == 0
    odd = jnp.logical_not(even)
    mate = jnp.where(even, z + 1, z - 1)
    lane = 128
    strips = hidden.shape[1] // lane

    def fetch(b):
        at = pl.ds(pl.multiple_of(b * lane, lane), lane)
        slot = lax.rem(b, 2)
        return [
            pltpu.make_async_copy(
                weights[i].at[:, at],
                strip.at[slot, :, pl.ds(i * lane, lane)],
                strip_in.at[slot, i],
            )
            for i in range(2)
        ]

    def late(first, last):
        def body(b, _):
            for copy in fetch(b):
                copy.wait()

            @pl.when(b + 1 < strips)
            def _():
                for copy in fetch(b + 1):
                    copy.start()

            at = pl.ds(pl.multiple_of(b * lane, lane), lane)
            both = jnp.dot(
                rows_late[...], strip[lax.rem(b, 2)], preferred_element_type=jnp.float32
            )
            both = both.astype(jnp.bfloat16).astype(jnp.float32)
            gate = both[:, :lane]
            width = conv.shape[0]
            position = lax.broadcasted_iota(jnp.int32, gate.shape, 0)
            pre = gate * conv[pl.ds(width - 1, 1), at]
            for j in range(width - 1):
                lag = width - 1 - j
                moved = jnp.where(position >= lag, pltpu.roll(gate, lag, 0), 0.0)
                pre = pre + moved * conv[pl.ds(j, 1), at]
            active = 0.5 * pre * (1.0 + lax.erf(pre * root_half))
            hidden[:, at] = (active * both[:, lane:]).astype(hidden.dtype)
            return 0

        lax.fori_loop(first, last, body, 0)

    def start_of(zz, yy):
        return pl.multiple_of((zz * 2 + yy) * rows, rows)

    def make(p, zz, yy):
        at = pl.ds(start_of(zz, yy), rows)
        term = jnp.dot(flipped[at, :], deltas[p][...], preferred_element_type=jnp.float32)
        terms[p][at, :] = (factor * term).astype(terms[p].dtype)

    def over(p, zz, source=None):
        return pltpu.make_async_remote_copy(
            src_ref=terms[p].at[pl.ds(start_of(zz, 1 - y), rows)] if source is None else source,
            dst_ref=y_got[p].at[zz],
            send_sem=y_out.at[p, zz],
            recv_sem=y_in.at[p, zz],
            device_id={"fs": z * 2 + 1 - y},
            device_id_type=MESH,
        )

    def along(p, zz, away, upward):
        got, sem = (up_got, up_in) if upward else (down_got, down_in)
        return pltpu.make_async_remote_copy(
            src_ref=y_got[p].at[zz],
            dst_ref=got[p].at[away - 1],
            send_sem=z_out.at[p, zz],
            recv_sem=sem.at[p, away - 1],
            device_id={"fs": (z + 1 if upward else z - 1) * 2 + y},
            device_id_type=MESH,
        )

    def cross():
        return pltpu.make_async_remote_copy(
            src_ref=terms[1].at[pl.ds(start_of(mate, 1 - y), rows)],
            dst_ref=cross_got,
            send_sem=cross_out,
            recv_sem=cross_in,
            device_id={"fs": mate * 2 + y},
            device_id_type=MESH,
        )

    def add_cross():
        base = start_of(z, 1 - y)

        def body(i, _):
            part = pl.ds(pl.multiple_of(i * step, step), step)
            value = terms[1][pl.ds(pl.multiple_of(base + i * step, step), step), :]
            value = value.astype(jnp.float32) + cross_got[part, :].astype(jnp.float32)
            cross_got[part, :] = value.astype(cross_got.dtype)
            return 0

        lax.fori_loop(0, rows // step, body, 0)

    def over_y(p, away, upward):
        if p == 1 and away == 1:
            return odd if upward else even
        return True

    def taps_copy(away):
        return pltpu.make_async_remote_copy(
            src_ref=taps,
            dst_ref=taps_got.at[me],
            send_sem=taps_out.at[away],
            recv_sem=taps_in.at[me],
            device_id={"fs": lax.rem(me + away, n)},
            device_id_type=MESH,
        )

    def add(p, zz, others, into, from_y=True):
        base = start_of(zz, y)

        def body(i, _):
            part = pl.ds(pl.multiple_of(i * step, step), step)
            value = terms[p][
                pl.ds(pl.multiple_of(base + i * step, step), step), :
            ].astype(jnp.float32)
            if from_y:
                value = value + y_got[p][zz, part, :].astype(jnp.float32)
            for ref, at in others:
                value = value + ref[at, part, :].astype(jnp.float32)
            if into is None:
                y_got[p][zz, part, :] = value.astype(y_got[p].dtype)
            else:
                into[part, :] = value.astype(into.dtype)
            return 0

        lax.fori_loop(0, rows // step, body, 0)

    for copy in fetch(0):
        copy.start()
    greet(n, me)
    make(1, mate, 1 - y)
    cross().start()

    def send_terms(i, _):
        away = depth - 1 - i
        for p in range(2):
            up_too = z + away < depth
            down_too = z - away >= 0
            if p == 1:
                up_too = jnp.logical_and(up_too, jnp.logical_or(away > 1, odd))
                down_too = jnp.logical_and(down_too, jnp.logical_or(away > 1, even))
            for here, zz in ((up_too, z + away), (down_too, z - away)):

                @pl.when(here)
                def _():
                    make(p, zz, 1 - y)
                    over(p, zz).start()

        return 0

    lax.fori_loop(0, depth - 1, send_terms, 0)
    make(0, z, 1 - y)
    over(0, z).start()
    for away in range(1, n):
        taps_copy(away).start()

    def pass_on(p, away, upward):
        zz = z + away if upward else z - away
        inside = zz < depth if upward else zz >= 0
        has_more = z > 0 if upward else z + 1 < depth
        got = up_got if upward else down_got
        kinds = [(True, True)]
        if p == 1 and away == 1:
            kinds = [(True, odd if upward else even), (False, even if upward else odd)]

        @pl.when(inside)
        def _():
            if away < depth - 1:
                pl.when(has_more)(lambda: along(p, zz, away + 1, upward).wait_recv())
            for from_y, here in kinds:

                @pl.when(jnp.logical_and(inside, here))
                def _():
                    if from_y:
                        over(p, zz).wait_recv()

                    @pl.when(has_more)
                    def _():
                        add(p, zz, [(got[p], away)] if away < depth - 1 else [], None, from_y)

                    @pl.when(jnp.logical_not(has_more))
                    def _():
                        add(p, zz, [], None, from_y)

            along(p, zz, away, upward).start()

    make(1, z, 1 - y)

    def own_terms(zz, _):
        for p in range(2):
            make(p, zz, y)
        return 0

    lax.fori_loop(0, depth, own_terms, 0)
    done = min(1, strips)
    late(0, done)
    for away in range(depth - 1, 0, -1):
        for p in range(2):
            pass_on(p, away, True)
            pass_on(p, away, False)
            if away == depth - 1 and p == 1:
                cross().wait_recv()
                add_cross()
                over(1, z, cross_got).start()
            if done < strips:
                upto = min(done + 2, strips)
                late(done, upto)
                done = upto
    if done < strips:
        late(done, strips)

    taps_got[pl.ds(me, 1)] = taps[...][None]
    for away in range(1, n):
        source = lax.rem(me + away, n)
        pltpu.make_async_remote_copy(
            src_ref=taps,
            dst_ref=taps_got.at[source],
            send_sem=taps_out.at[away],
            recv_sem=taps_in.at[source],
            device_id={"fs": source},
            device_id_type=MESH,
        ).wait_recv()
    sum_of = taps_got[0]
    for i in range(1, n):
        sum_of = sum_of + taps_got[i]
    taps_total[...] = sum_of

    for p in range(2):
        over(p, z).wait_recv()
        pl.when(z > 0)(lambda: along(p, z, 1, True).wait_recv())
        pl.when(z + 1 < depth)(lambda: along(p, z, 1, False).wait_recv())
        at_low, at_high = z == 0, z + 1 == depth
        both = jnp.logical_not(jnp.logical_or(at_low, at_high))
        pl.when(at_low)(lambda: add(p, z, [(down_got[p], 0)], total[p]))
        pl.when(at_high)(lambda: add(p, z, [(up_got[p], 0)], total[p]))
        pl.when(both)(lambda: add(p, z, [(up_got[p], 0), (down_got[p], 0)], total[p]))

    cross().wait_send()
    over(0, z).wait_send()
    over(1, z, cross_got).wait_send()
    for p in range(2):
        for away in range(depth - 1, 0, -1):
            up_too, down_too = over_y(p, away, True), over_y(p, away, False)

            @pl.when(z + away < depth)
            def _():
                pl.when(jnp.logical_and(z + away < depth, up_too))(
                    lambda: over(p, z + away).wait_send()
                )
                along(p, z + away, away, True).wait_send()

            @pl.when(z - away >= 0)
            def _():
                pl.when(jnp.logical_and(z - away >= 0, down_too))(
                    lambda: over(p, z - away).wait_send()
                )
                along(p, z - away, away, False).wait_send()

    for away in range(1, n):
        taps_copy(away).wait_send()


def scatter_rows(factor, flipped, d_gate, d_value, tap_terms, rows_late, gate_full, value_full, conv_taps):
    n = lax.axis_size("fs")
    depth = n // 2
    rows, columns = flipped.shape[0] // n, d_gate.shape[1]
    sems = pltpu.SemaphoreType.DMA
    vmem = pl.BlockSpec(memory_space=pltpu.VMEM)
    total = jax.ShapeDtypeStruct((rows, columns), jnp.float32)
    row_block = lambda count: pltpu.VMEM((count, rows, columns), d_gate.dtype)
    return pl.pallas_call(
        functools.partial(scatter_kernel, n, factor),
        out_shape=(
            total,
            total,
            jax.ShapeDtypeStruct(tap_terms.shape, jnp.float32),
            jax.ShapeDtypeStruct((rows_late.shape[0], columns), jnp.bfloat16),
        ),
        in_specs=[vmem] * 5 + [pl.BlockSpec(memory_space=pl.ANY)] * 2 + [vmem],
        out_specs=(vmem,) * 4,
        scratch_shapes=[row_block(depth)] * 2
        + [row_block(depth - 1)] * 4
        + [
            pltpu.VMEM((n,) + tap_terms.shape, jnp.float32),
            pltpu.VMEM((rows, columns), d_gate.dtype),
            pltpu.VMEM((2, gate_full.shape[0], 256), gate_full.dtype),
            pltpu.VMEM((n * rows, columns), d_gate.dtype),
            pltpu.VMEM((n * rows, columns), d_gate.dtype),
            sems((2, depth)),
            sems((2, depth)),
            sems((2, depth)),
            sems((2, depth)),
            sems((2, depth)),
            sems((n,)),
            sems((n,)),
            sems,
            sems,
            sems((2, 2)),
        ],
        compiler_params=pltpu.CompilerParams(
            collective_id=1, has_side_effects=True, vmem_limit_bytes=60 * 1024 * 1024
        ),
        name="scatter_rows",
    )(flipped, d_gate, d_value, tap_terms, rows_late, gate_full, value_full, conv_taps)


def shards(x_late, x_early, w_gate, w_value, conv_taps, grad_hidden, sum_gate, sum_value, sum_taps):
    columns = w_gate.shape[1]
    factor = 1.0 / math.sqrt(x_late.shape[0] * lax.axis_size("fs") * lax.axis_size("tp"))
    gate_full, value_full = gather_rows(w_gate, w_value)
    block_rows = lax.all_gather(x_late, "tp", axis=0, tiled=True)
    gathered = lax.all_gather(x_early, "tp", axis=0, tiled=True)
    gate_rows = jnp.dot(gathered, gate_full, preferred_element_type=jnp.float32).astype(
        jnp.bfloat16
    )
    value_rows = jnp.dot(gathered, value_full, preferred_element_type=jnp.float32).astype(
        jnp.bfloat16
    )
    mixed_pre, padded = causal_mix(gate_rows, conv_taps)
    upstream = grad_hidden.astype(jnp.float32)
    slope_rows = upstream * value_rows.astype(jnp.float32) * gelu_slope(mixed_pre)
    d_gate_f, tap_terms = back_mix(slope_rows, conv_taps, padded)
    d_gate = d_gate_f.astype(jnp.bfloat16)
    d_value = (upstream * jax.nn.gelu(mixed_pre, approximate=False)).astype(jnp.bfloat16)
    contract = (((1,), (1,)), ((), ()))
    grad_early = lax.psum_scatter(
        (
            lax.dot_general(d_gate, gate_full, contract, preferred_element_type=jnp.float32)
            + lax.dot_general(d_value, value_full, contract, preferred_element_type=jnp.float32)
        ).astype(jnp.bfloat16),
        "tp",
        scatter_dimension=0,
        tiled=True,
    )
    taps_padded = jnp.pad(factor * tap_terms, ((0, -tap_terms.shape[0] % 8), (0, 0)))
    gate_total, value_total, tap_total, hidden = scatter_rows(
        factor,
        gathered.T,
        d_gate,
        d_value,
        taps_padded,
        block_rows,
        gate_full,
        value_full,
        conv_taps,
    )
    tap_total = tap_total[: tap_terms.shape[0]]
    return (
        hidden,
        grad_early,
        sum_gate + gate_total,
        sum_value + value_total,
        sum_taps + tap_total,
    )


def solution(mesh):
    placed = (
        P(("fs", "tp"), None),
        P(("fs", "tp"), None),
        P("fs", "tp"),
        P("fs", "tp"),
        P(None, "tp"),
        P("fs", "tp"),
        P("fs", "tp"),
        P("fs", "tp"),
        P(None, "tp"),
    )
    return jax.shard_map(
        shards,
        mesh=mesh,
        in_specs=placed,
        out_specs=(
            P("fs", "tp"),
            P(("fs", "tp"), None),
            P("fs", "tp"),
            P("fs", "tp"),
            P(None, "tp"),
        ),
        check_vma=False,
    )
```
